32 devices in a mesh: dp: 4 (over y, x), kv: 4 (over z), tp: 2 (over core).
Axes of the slice: x: 2, y: 2, z: 4, core: 2. Of those that a mesh axis runs over, the one named last changes fastest.
Arguments:
- tokens: bfloat16 [128, 2048], P('dp', ('kv', 'tp')), may hold values from -60 to 60
- first_norm_gain: float32 [2048], replicated, may hold values from 0.1 to 1.9
- first_gate_weight: bfloat16 [2048, 5632], P(None, ('kv', 'tp')), may hold values from -0.125 to 0.125
- first_up_weight: bfloat16 [2048, 5632], P(None, ('kv', 'tp')), may hold values from -0.125 to 0.125
- first_down_weight: bfloat16 [5632, 2048], P(('kv', 'tp')), may hold values from -0.109375 to 0.109375
- mixer_norm_gain: float32 [2048], replicated, may hold values from 0.1 to 1.9
- query_weight: bfloat16 [2048, 1024], P('kv', 'tp'), may hold values from -0.125 to 0.125
- key_weight: bfloat16 [2048, 1024], P('kv', 'tp'), may hold values from -0.125 to 0.125
- value_weight: bfloat16 [2048, 1024], P('kv', 'tp'), may hold values from -0.125 to 0.125
- output_gate_weight: bfloat16 [2048, 1024], P('kv', 'tp'), may hold values from -0.125 to 0.125
- strength_weight: bfloat16 [2048, 8], replicated, may hold values from -0.125 to 0.125
- decay_weight: bfloat16 [2048, 8], replicated, may hold values from -0.125 to 0.125
- head_decay_log: float32 [8], replicated, may hold values from 0 to 2.77
- decay_input_bias: float32 [8], replicated, may hold values from -4 to 0
- decay_extra_log: float32 [128, 8], P(('dp', 'kv'), 'tp'), may hold values from -0.7 to 0
- head_norm_gain: float32 [128], replicated, may hold values from 0.1 to 1.9
- state: float32 [128, 8, 128, 128], P(('dp', 'kv'), 'tp'), may hold values from -0.6 to 0.6
- mixer_output_weight: bfloat16 [1024, 2048], P('tp', 'kv'), may hold values from -0.1875 to 0.1875
- second_norm_gain: float32 [2048], replicated, may hold values from 0.1 to 1.9
- second_gate_weight: bfloat16 [2048, 5632], P(None, ('kv', 'tp')), may hold values from -0.125 to 0.125
- second_up_weight: bfloat16 [2048, 5632], P(None, ('kv', 'tp')), may hold values from -0.125 to 0.125
- second_down_weight: bfloat16 [5632, 2048], P(('kv', 'tp')), may hold values from -0.109375 to 0.109375
Outputs:
- layer_out: bfloat16 [128, 2048], P('dp', ('kv', 'tp'))
- new_state: float32 [128, 8, 128, 128], P(('dp', 'kv'), 'tp')
The draws below stay inside these ranges and needn't reach their ends.
All inputs are finite; a program needn't handle non-finite values.
Results may differ from the reference program's by a relative error of at most 0.014.
Values may be sent and summed in bfloat16 or wider, within the bound.
A program may use at most 64 MiB of HBM per device.

```python
import jax
import jax.numpy as jnp
from jax import lax

D = 2048
FF = 5632
MIXER_HEADS = 8
HEAD_DIM = 128
SEQUENCE_COUNT = 128
N_TP = 2


def draw_tokens(key, part):
    base_key = jax.random.fold_in(key, 11)
    jitter_key = jax.random.fold_in(key, 12)
    rows_key = jax.random.fold_in(key, 13)
    column_pos = jnp.arange(D, dtype=jnp.float32) / D
    rising = 0.45 * jnp.exp(jnp.log(5.0) * column_pos)
    jitter = jnp.exp(jax.random.uniform(jitter_key, (D,), jnp.float32, -0.5, 0.5))
    row_scales = jnp.exp(jax.random.uniform(rows_key, (SEQUENCE_COUNT, 1), jnp.float32, -1.15, 1.15))
    base = jnp.clip(jax.random.normal(base_key, (SEQUENCE_COUNT, D), jnp.float32), -4.0, 4.0)
    return (base * rising * jitter * row_scales).astype(jnp.bfloat16)


def strengthened(drawn, rng, source, target, shards_of, factor):
    owner, partner = [(jnp.arange(drawn.shape[position]) // (drawn.shape[position] // shards_of)).reshape([-1 if axis == position else 1 for axis in range(drawn.ndim)]) for position in (source, target)]
    chosen = jax.random.permutation(rng, shards_of)[partner]
    strong = (owner == chosen) | (owner == (partner + shards_of // 2) % shards_of)
    return jnp.where(strong, factor * drawn, drawn)


def level_of(own_key, shape, split, low, high):
    def one(axis_at, blocks):
        draws = jax.random.uniform(jax.random.fold_in(jax.random.fold_in(own_key, 6), axis_at), (blocks,), jnp.float32, low / len(split), high / len(split))
        return jnp.repeat(jnp.exp(draws), shape[axis_at] // blocks).reshape((-1,) + (1,) * (len(shape) - axis_at - 1))

    gain = one(*split[0])
    for cut in split[1:]:
        gain = gain * one(*cut)
    return gain


def noise(own_key, dims, width, most, shards=(), held_as=jnp.bfloat16):
    level = level_of(own_key, dims, shards, -0.22, 0.18) if shards else 1.0
    array = jax.random.normal(own_key, dims, jnp.float32) * width * level
    return jnp.minimum(jnp.maximum(array, -most), most).astype(held_as)


def noise_with(rng, shape, spread, limit, cuts, heavy, held_as=jnp.bfloat16):
    array = spread * jax.random.normal(rng, shape, jnp.float32)
    if cuts:
        array = array * level_of(rng, shape, cuts, -0.22, 0.18)
    return jnp.clip(strengthened(array, jax.random.fold_in(rng, 3), *heavy), -limit, limit).astype(held_as)


def setup_inputs(seed: int = 0) -> dict:
    splits = jax.random.split(jax.random.key(seed), 23)
    return {
        "tokens": draw_tokens(jax.random.fold_in(splits[22], 71), 0),
        "first_norm_gain": jnp.clip(1.0 + 0.18 * jax.random.normal(splits[1], (D,), jnp.float32), 0.1, 1.9),
        "first_gate_weight": noise(splits[2], (D, FF), D ** -0.5, 0.125, ((1, 8),)),
        "first_up_weight": noise(splits[3], (D, FF), D ** -0.5, 0.125, ((1, 8),)),
        "first_down_weight": noise_with(splits[4], (FF, D), FF ** -0.5, 0.109375, ((0, 8),), (0, 1, 8, 2.0)),
        "mixer_norm_gain": jnp.clip(1.0 + 0.18 * jax.random.normal(splits[5], (D,), jnp.float32), 0.1, 1.9),
        "query_weight": noise(splits[6], (D, MIXER_HEADS * HEAD_DIM), D ** -0.5, 0.125, ((0, 4), (1, 2))),
        "key_weight": noise(splits[7], (D, MIXER_HEADS * HEAD_DIM), D ** -0.5, 0.125, ((0, 4), (1, 2))),
        "value_weight": noise(splits[8], (D, MIXER_HEADS * HEAD_DIM), D ** -0.5, 0.125, ((0, 4), (1, 2))),
        "output_gate_weight": noise(splits[9], (D, MIXER_HEADS * HEAD_DIM), D ** -0.5, 0.125, ((0, 4), (1, 2))),
        "strength_weight": noise(splits[10], (D, MIXER_HEADS), D ** -0.5, 0.125),
        "decay_weight": noise(splits[11], (D, MIXER_HEADS), D ** -0.5, 0.125),
        "head_decay_log": jnp.clip(jax.random.uniform(splits[12], (MIXER_HEADS,), jnp.float32, 0.0, 2.77), 0.0, 2.77),
        "decay_input_bias": jnp.clip(jax.random.uniform(splits[13], (MIXER_HEADS,), jnp.float32, -4.0, 0.0), -4.0, 0.0),
        "decay_extra_log": jnp.clip(-0.7 + 0.7 * jax.random.uniform(splits[14], (SEQUENCE_COUNT, MIXER_HEADS), jnp.float32) ** level_of(splits[14], (SEQUENCE_COUNT, MIXER_HEADS), ((0, 16), (1, 2)), -0.2, 0.2), -0.7, 0.0),
        "head_norm_gain": jnp.clip(1.0 + 0.18 * jax.random.normal(splits[15], (HEAD_DIM,), jnp.float32), 0.1, 1.9),
        "state": noise(splits[16], (SEQUENCE_COUNT, MIXER_HEADS, HEAD_DIM, HEAD_DIM), 0.1, 0.6, ((0, 16), (1, 2)), jnp.float32),
        "mixer_output_weight": noise(splits[17], (MIXER_HEADS * HEAD_DIM, D), (MIXER_HEADS * HEAD_DIM) ** -0.5, 0.1875, ((0, 2), (1, 4))),
        "second_norm_gain": jnp.clip(1.0 + 0.18 * jax.random.normal(splits[18], (D,), jnp.float32), 0.1, 1.9),
        "second_gate_weight": noise(splits[19], (D, FF), D ** -0.5, 0.125, ((1, 8),)),
        "second_up_weight": noise(splits[20], (D, FF), D ** -0.5, 0.125, ((1, 8),)),
        "second_down_weight": noise_with(splits[21], (FF, D), FF ** -0.5, 0.109375, ((0, 8),), (0, 1, 8, 2.0)),
    }


EPS = 1e-06

def row_scale(values):
    return lax.rsqrt(lax.optimization_barrier(jnp.mean(values * values, axis=-1, keepdims=True)) + EPS)

def unit_rows(values):
    return values * lax.rsqrt(lax.optimization_barrier(jnp.sum(values * values, axis=-1, keepdims=True)) + EPS)

def half_block(row_data, gain_vec, w_gate, w_up, w_down):
    rows32 = row_data.astype(jnp.float32)
    normed = (rows32 * row_scale(rows32) * gain_vec).astype(jnp.bfloat16)
    gate_pre = jnp.dot(normed, w_gate, preferred_element_type=jnp.float32)
    upward = jnp.dot(normed, w_up, preferred_element_type=jnp.float32)
    hidden = (jax.nn.silu(gate_pre) * upward).astype(jnp.bfloat16)
    return jnp.dot(hidden, w_down, preferred_element_type=jnp.float32)

def delta_step(query_vec, key_vec, value_vec, gate_vals, beta_gate, head_decay_rate, state, head_norm_gain):
    recalled = jnp.einsum('shd,shde->she', key_vec, state, precision=lax.Precision.HIGHEST)
    correction = beta_gate[..., None] * (value_vec - head_decay_rate[..., None] * recalled)
    new_state = head_decay_rate[..., None, None] * state + key_vec[..., :, None] * correction[..., None, :]
    read_out = jnp.einsum('shd,shde->she', query_vec, new_state, precision=lax.Precision.HIGHEST)
    normed = read_out * row_scale(read_out) * head_norm_gain
    return (normed * jax.nn.silu(gate_vals), new_state)

def reference(tokens, first_norm_gain, first_gate_weight, first_up_weight, first_down_weight, mixer_norm_gain, query_weight, key_weight, value_weight, output_gate_weight, strength_weight, decay_weight, head_decay_log, decay_input_bias, decay_extra_log, head_norm_gain, state, mixer_output_weight, second_norm_gain, second_gate_weight, second_up_weight, second_down_weight):
    batch_rows = tokens.shape[0]
    first_rows = (tokens.astype(jnp.float32) + 0.5 * half_block(tokens, first_norm_gain, first_gate_weight, first_up_weight, first_down_weight)).astype(jnp.bfloat16)
    first32 = first_rows.astype(jnp.float32)
    row_factor = row_scale(first32)
    scaled_rows = (first32 * mixer_norm_gain).astype(jnp.bfloat16)

    def apply_projection(weight):
        return row_factor * jnp.dot(scaled_rows, weight, preferred_element_type=jnp.float32)

    def split_heads(values):
        return values.reshape(batch_rows, MIXER_HEADS, HEAD_DIM)
    query_vec = unit_rows(jax.nn.silu(split_heads(apply_projection(query_weight)))) * HEAD_DIM ** (-0.5)
    key_vec = unit_rows(jax.nn.silu(split_heads(apply_projection(key_weight))))
    value_vec = jax.nn.silu(split_heads(apply_projection(value_weight)))
    gate_vals = split_heads(apply_projection(output_gate_weight))
    beta_gate = jax.nn.sigmoid(apply_projection(strength_weight))
    head_decay_rate = jnp.exp(decay_extra_log - jnp.exp(head_decay_log) * jax.nn.softplus(apply_projection(decay_weight) + decay_input_bias))
    heads_f32, new_state = delta_step(query_vec, key_vec, value_vec, gate_vals, beta_gate, head_decay_rate, state, head_norm_gain)
    heads_out = heads_f32.reshape(batch_rows, N_TP, MIXER_HEADS * HEAD_DIM // N_TP).astype(jnp.bfloat16)
    w_parts = mixer_output_weight.reshape(N_TP, MIXER_HEADS * HEAD_DIM // N_TP, D)
    mixer_sum = jnp.zeros((batch_rows, D), jnp.float32)
    for tp_part in range(N_TP):
        partial_value = jnp.dot(heads_out[:, tp_part], w_parts[tp_part], preferred_element_type=jnp.float32).astype(jnp.bfloat16)
        partial_value = lax.optimization_barrier(partial_value)
        mixer_sum = mixer_sum + partial_value.astype(jnp.float32)
    second_rows = (first32 + mixer_sum).astype(jnp.bfloat16)
    layer_out = (second_rows.astype(jnp.float32) + 0.5 * half_block(second_rows, second_norm_gain, second_gate_weight, second_up_weight, second_down_weight)).astype(jnp.bfloat16)
    return (layer_out, new_state)
```

```python
import functools

import jax
import jax.numpy as jnp
from jax import lax
from jax.experimental import pallas as pl
from jax.experimental.pallas import tpu as pltpu
from jax.sharding import PartitionSpec as P

EPS = 1e-06


def row_scale(values):
    return lax.rsqrt(jnp.mean(values * values, axis=-1, keepdims=True) + EPS)


def unit_rows(values):
    return values * lax.rsqrt(jnp.sum(values * values, axis=-1, keepdims=True) + EPS)


def block_terms(row_data, gain_vec, w_gate, w_up, w_down):
    rows32 = row_data.astype(jnp.float32)
    normed = (rows32 * row_scale(rows32) * gain_vec).astype(jnp.bfloat16)
    gate_pre = jnp.dot(normed, w_gate, preferred_element_type=jnp.float32)
    upward = jnp.dot(normed, w_up, preferred_element_type=jnp.float32)
    hidden = (jax.nn.silu(gate_pre) * upward).astype(jnp.bfloat16)
    return jnp.dot(hidden, w_down, preferred_element_type=jnp.float32)


def delta_step(
    query_vec, key_vec, value_vec, gate_vals, beta_gate, head_decay_rate, state, head_norm_gain
):
    recalled = jnp.einsum("shd,shde->she", key_vec, state, precision=lax.Precision.HIGHEST)
    correction = beta_gate[..., None] * (value_vec - head_decay_rate[..., None] * recalled)
    new_state = (
        head_decay_rate[..., None, None] * state + key_vec[..., :, None] * correction[..., None, :]
    )
    read_out = jnp.einsum("shd,shde->she", query_vec, new_state, precision=lax.Precision.HIGHEST)
    normed = read_out * row_scale(read_out) * head_norm_gain
    return (normed * jax.nn.silu(gate_vals), new_state)


def shards_plain(
    tokens,
    first_norm_gain,
    first_gate_weight,
    first_up_weight,
    first_down_weight,
    mixer_norm_gain,
    query_weight,
    key_weight,
    value_weight,
    output_gate_weight,
    strength_weight,
    decay_weight,
    head_decay_log,
    decay_input_bias,
    decay_extra_log,
    head_norm_gain,
    state,
    mixer_output_weight,
    second_norm_gain,
    second_gate_weight,
    second_up_weight,
    second_down_weight,
):
    batch_rows, columns = tokens.shape
    kv_index = lax.axis_index("kv")
    tp_index = lax.axis_index("tp")
    own_block = kv_index * lax.axis_size("tp") + tp_index
    seq_dev, heads_dev, head_size = (state.shape[0], state.shape[1], state.shape[2])
    kv_width = query_weight.shape[0]
    head_cols = heads_dev * head_size
    model_width = mixer_norm_gain.shape[0]
    rows_all = lax.all_gather(tokens, ("kv", "tp"), axis=1, tiled=True)
    ffn_terms = block_terms(
        rows_all, first_norm_gain, first_gate_weight, first_up_weight, first_down_weight
    )
    share_sum = lax.psum_scatter(
        ffn_terms.astype(jnp.bfloat16), ("kv", "tp"), scatter_dimension=1, tiled=True
    ).astype(jnp.float32)
    first_rows = (tokens.astype(jnp.float32) + 0.5 * share_sum).astype(jnp.bfloat16)
    first32 = first_rows.astype(jnp.float32)
    kv_block = lax.all_gather(first_rows, "tp", axis=1, tiled=True)
    own_gain = lax.dynamic_slice_in_dim(mixer_norm_gain, own_block * columns, columns)
    own_scaled = (first32 * own_gain).astype(jnp.bfloat16)
    beta_rows = lax.dynamic_slice_in_dim(strength_weight, own_block * columns, columns, 0)
    decay_rows = lax.dynamic_slice_in_dim(decay_weight, own_block * columns, columns, 0)
    squares, beta_pre, decay_logits = lax.psum(
        (
            jnp.sum(first32 * first32, axis=1),
            jnp.dot(own_scaled, beta_rows, preferred_element_type=jnp.float32),
            jnp.dot(own_scaled, decay_rows, preferred_element_type=jnp.float32),
        ),
        ("kv", "tp"),
    )
    row_factor = lax.rsqrt(squares / model_width + EPS)
    block_gain = lax.dynamic_slice_in_dim(mixer_norm_gain, kv_index * kv_width, kv_width)
    block_scaled = (kv_block.astype(jnp.float32) * block_gain).astype(jnp.bfloat16)
    projected = lax.psum_scatter(
        jnp.concatenate(
            [
                jnp.dot(block_scaled, weight, preferred_element_type=jnp.float32)
                for weight in (query_weight, key_weight, value_weight, output_gate_weight)
            ],
            axis=1,
        ).astype(jnp.bfloat16),
        "kv",
        scatter_dimension=0,
        tiled=True,
    ).astype(jnp.float32)
    own_rows = kv_index * seq_dev
    own_factor = lax.dynamic_slice_in_dim(row_factor, own_rows, seq_dev)[:, None]
    projected = projected * own_factor

    def split_heads(role_index):
        return projected[:, role_index * head_cols : (role_index + 1) * head_cols].reshape(
            seq_dev, heads_dev, head_size
        )

    query_vec = unit_rows(jax.nn.silu(split_heads(0))) * head_size ** (-0.5)
    key_vec = unit_rows(jax.nn.silu(split_heads(1)))
    value_vec = jax.nn.silu(split_heads(2))
    gate_vals = split_heads(3)
    head_start = tp_index * heads_dev

    def local_gate_values(values):
        own_seqs = lax.dynamic_slice_in_dim(values, own_rows, seq_dev, 0)
        return lax.dynamic_slice_in_dim(own_seqs, head_start, heads_dev, 1) * own_factor

    beta_gate = jax.nn.sigmoid(local_gate_values(beta_pre))
    decay_log_term = lax.dynamic_slice_in_dim(head_decay_log, head_start, heads_dev)
    decay_offset_term = lax.dynamic_slice_in_dim(decay_input_bias, head_start, heads_dev)
    head_decay_rate = jnp.exp(
        decay_extra_log
        - jnp.exp(decay_log_term)
        * jax.nn.softplus(local_gate_values(decay_logits) + decay_offset_term)
    )
    heads_f32, new_state = delta_step(
        query_vec, key_vec, value_vec, gate_vals, beta_gate, head_decay_rate, state, head_norm_gain
    )
    heads_out = heads_f32.reshape(seq_dev, head_cols).astype(jnp.bfloat16)
    mixer_terms = jnp.dot(
        lax.all_gather(heads_out, "kv", axis=0, tiled=True),
        mixer_output_weight,
        preferred_element_type=jnp.float32,
    )
    mixer_sum = lax.psum_scatter(
        mixer_terms.astype(jnp.bfloat16), "tp", scatter_dimension=1, tiled=True
    ).astype(jnp.float32)
    second_rows = (first32 + mixer_sum).astype(jnp.bfloat16)
    rows_last = lax.all_gather(second_rows, ("kv", "tp"), axis=1, tiled=True)
    last_terms = block_terms(
        rows_last, second_norm_gain, second_gate_weight, second_up_weight, second_down_weight
    )
    last_sum = lax.psum_scatter(
        last_terms.astype(jnp.bfloat16), ("kv", "tp"), scatter_dimension=1, tiled=True
    ).astype(jnp.float32)
    layer_out = (second_rows.astype(jnp.float32) + 0.5 * last_sum).astype(jnp.bfloat16)
    return (layer_out, new_state)


MESH = pl.DeviceIdType.MESH
BF16 = jnp.bfloat16
F32 = jnp.float32


def dot32(a, b):
    return jnp.dot(a, b, preferred_element_type=F32)


def silu(x):
    return x * jax.nn.sigmoid(x)


def layer_kernel(nkv, ntp, *refs):
    (tok_h, gain1_h, wg1_h, wu1_h, wd1_h, mgain_h, wq_h, wk_h, wv_h, wo_h, ws_h, wdec_h,
     hlog_h, bias_h, extra_h, hgain_h, state_h, wout_h, gain2_h, wg2_h, wu2_h, wd2_h,
     out_h, new_h,
     gain1, wg1, wu1, wd1, mgain, wq, wk, wv, wo, ws, wdec, hlog, bias, extra, hgain,
     state, wout, gain2, wg2, wu2, wd2,
     gath1, gath2, gath3, part1, recv1, part2, recv2, projs, projr, heads_g, halves, halfr,
     gates_v, ks_v, qs_v, newst, out_v, load_sem, out_sem, send_sem, recv_sem) = refs
    n = nkv * ntp
    kv = lax.axis_index("kv")
    tp = lax.axis_index("tp")
    me = kv * ntp + tp
    rows, cols = tok_h.shape
    seqs, heads, hd, _ = state_h.shape
    width = heads * hd
    model = n * cols

    tok_copy = pltpu.make_async_copy(tok_h, gath1.at[me], load_sem.at[0])
    tok_copy.start()
    order = [(gain1_h, gain1), (wg1_h, wg1), (wu1_h, wu1), (wd1_h, wd1), (mgain_h, mgain),
             (wq_h, wq), (wk_h, wk), (wv_h, wv), (wo_h, wo), (ws_h, ws), (wdec_h, wdec),
             (hlog_h, hlog), (bias_h, bias), (extra_h, extra), (hgain_h, hgain),
             (state_h, state), (wout_h, wout), (gain2_h, gain2), (wg2_h, wg2),
             (wu2_h, wu2), (wd2_h, wd2)]
    loads = {}
    for at, (source, dest) in enumerate(order):
        copy = pltpu.make_async_copy(source, dest, load_sem.at[at + 1])
        copy.start()
        loads[id(dest)] = copy

    def need(*dests):
        for dest in dests:
            loads[id(dest)].wait()

    def peer(step):
        to_kv = lax.rem(kv + step // ntp, nkv)
        to_tp = lax.rem(tp + step % ntp, ntp)
        return to_kv * ntp + to_tp, {"kv": to_kv, "tp": to_tp}

    def origin(step):
        return lax.rem(kv + nkv - step // ntp, nkv) * ntp + lax.rem(tp + ntp - step % ntp, ntp)

    barrier = pltpu.get_barrier_semaphore()
    for step in range(1, n):
        pl.semaphore_signal(barrier, inc=1, device_id=peer(step)[1], device_id_type=MESH)
    pl.semaphore_wait(barrier, n - 1)

    def send(source, dest, phase, step):
        copy = pltpu.make_async_remote_copy(
            src_ref=source, dst_ref=dest, send_sem=send_sem.at[phase, step],
            recv_sem=recv_sem.at[phase, step], device_id=peer(step)[1], device_id_type=MESH)
        copy.start()
        return copy

    def spread(gath, phase):
        return {step: send(gath.at[me], gath.at[me], phase, step) for step in range(1, n)}

    def block_of(at):
        return pl.ds(pl.multiple_of(at * cols, cols), cols)

    def half_block(gath, copies, gain, w_gate, w_up, w_down, part, recv, phase):
        def take(source, carry):
            squares, gate, up = carry
            block = gath[source].astype(F32)
            squares = squares + jnp.sum(block * block, axis=1, keepdims=True)
            scaled = (block * gain[:, block_of(source)]).astype(BF16)
            gate = gate + dot32(scaled, w_gate[block_of(source), :])
            up = up + dot32(scaled, w_up[block_of(source), :])
            return (squares, gate, up)

        hidden_cols = w_gate.shape[1]
        need(gain, w_gate, w_up)
        zeros = jnp.zeros((rows, hidden_cols), F32)
        carry = take(me, (jnp.zeros((rows, 1), F32), zeros, zeros))
        for step in range(1, n):
            copies[step].wait()
            carry = take(origin(step), carry)
        squares, gate, up = carry
        factor = lax.rsqrt(squares / model + EPS)
        hidden = (silu(gate * factor) * (up * factor)).astype(BF16)
        need(w_down)
        sends = {}
        for step in range(1, n):
            part[step - 1] = dot32(hidden, w_down[:, block_of(peer(step)[0])]).astype(BF16)
            sends[step] = send(part.at[step - 1], recv.at[step - 1], phase, step)
        total = dot32(hidden, w_down[:, block_of(me)])
        for step in range(1, n):
            sends[step].wait()
            total = total + recv[step - 1].astype(F32)
        return total

    tok_copy.wait()
    copies = spread(gath1, 0)
    share = half_block(gath1, copies, gain1, wg1, wu1, wd1, part1, recv1, 1)
    first = (gath1[me].astype(F32) + 0.5 * share).astype(BF16)
    gath2[me] = first
    copies = spread(gath2, 2)

    def scaled_block(source):
        return (gath2[source].astype(F32) * mgain[:, block_of(source)]).astype(BF16)

    need(mgain, wq, wk, wv, wo)
    acc = [jnp.zeros((rows, width), F32) for _ in range(4)]
    for step in range(ntp):
        if step:
            copies[step].wait()
        source = origin(step)
        local = block_of(lax.rem(source, ntp))
        scaled = scaled_block(source)
        acc = [a + dot32(scaled, w[local, :]) for a, w in zip(acc, (wq, wk, wv, wo))]
    for role in range(4):
        projs[:, :, role * width:(role + 1) * width] = acc[role].reshape(nkv, seqs, width).astype(BF16)
    psends = {}
    for dk in range(1, nkv):
        to_kv = lax.rem(kv + dk, nkv)
        psends[dk] = send(projs.at[to_kv], projr.at[dk - 1], 3, dk * ntp)

    need(ws, wdec, hlog, bias, extra, hgain)
    squares = jnp.zeros((rows, 1), F32)
    beta_all = jnp.zeros((rows, ws.shape[1]), F32)
    dec_all = jnp.zeros((rows, ws.shape[1]), F32)
    for step in range(n):
        if step >= ntp:
            copies[step].wait()
        source = origin(step)
        block = gath2[source].astype(F32)
        squares = squares + jnp.sum(block * block, axis=1, keepdims=True)
        scaled = scaled_block(source)
        beta_all = beta_all + dot32(scaled, ws[block_of(source), :])
        dec_all = dec_all + dot32(scaled, wdec[block_of(source), :])
    gates_v[0] = jnp.broadcast_to(lax.rsqrt(squares / model + EPS), (rows, 128))
    gates_v[1, :, 0:ws.shape[1]] = beta_all
    gates_v[2, :, 0:ws.shape[1]] = dec_all
    own = pl.ds(pl.multiple_of(kv * seqs, seqs), seqs)
    factor = gates_v[0, own, :][:, 0:1]

    def own_heads(values):
        picked = values[:, 0:heads]
        for at in range(1, ntp):
            picked = jnp.where(tp == at, values[:, at * heads:(at + 1) * heads], picked)
        return picked

    beta = jax.nn.sigmoid(own_heads(gates_v[1, own, :]) * factor)
    logits = own_heads(gates_v[2, own, :]) * factor + own_heads(bias[...])
    softplus = jnp.maximum(logits, 0.0) + jnp.log1p(jnp.exp(-jnp.abs(logits)))
    decay = jnp.exp(extra[...] - jnp.exp(own_heads(hlog[...])) * softplus)

    summed = projs[kv].astype(F32)
    for dk in range(1, nkv):
        psends[dk].wait()
        summed = summed + projr[dk - 1].astype(F32)
    summed = summed * factor

    def role_head(role, h):
        start = role * width + h * hd
        return summed[:, start:start + hd]

    def unit(u):
        return u * lax.rsqrt(jnp.sum(u * u, axis=-1, keepdims=True) + EPS)

    key_h = [unit(silu(role_head(1, h))) for h in range(heads)]
    query_hs = [unit(silu(role_head(0, h))) * hd ** (-0.5) for h in range(heads)]
    pad = jnp.zeros((hd - 2 * heads * seqs, hd), F32)
    turned = jnp.concatenate(key_h + query_hs + [pad], axis=0).T
    need(state)
    for h in range(heads):
        for s in range(seqs):
            mat = state[s, h]
            at = h * seqs + s
            ks_v[h, s:s + 1, :] = jnp.sum(turned[:, at:at + 1] * mat, axis=0, keepdims=True)
            at = at + heads * seqs
            qs_v[h, s:s + 1, :] = jnp.sum(turned[:, at:at + 1] * mat, axis=0, keepdims=True)
    corrections = []
    decays = []
    outs = []
    for h in range(heads):
        rate = jnp.broadcast_to(decay[:, h:h + 1], (seqs, hd))
        correction = beta[:, h:h + 1] * (silu(role_head(2, h)) - rate * ks_v[h])
        mix = jnp.sum(query_hs[h] * key_h[h], axis=1, keepdims=True)
        read = rate * qs_v[h] + mix * correction
        normed = read * lax.rsqrt(jnp.mean(read * read, axis=-1, keepdims=True) + EPS) * hgain[...]
        outs.append((normed * silu(role_head(3, h))).astype(BF16))
        corrections.append(correction)
        decays.append(rate)
    for h in range(heads):
        heads_g[kv, :, h * hd:(h + 1) * hd] = outs[h]
    hsends = {dk: send(heads_g.at[kv], heads_g.at[kv], 4, dk * ntp) for dk in range(1, nkv)}

    for h in range(heads):
        ks_v[h] = corrections[h]
        qs_v[h] = decays[h]
    for h in range(heads):
        for s in range(seqs):
            at = h * seqs + s
            newst[s, h] = qs_v[h, s:s + 1, :] * state[s, h] + turned[:, at:at + 1] * ks_v[h, s:s + 1, :]
    state_copy = pltpu.make_async_copy(newst, new_h, out_sem.at[0])
    state_copy.start()

    need(wout)
    for dk in range(1, nkv):
        hsends[dk].wait()
    all_heads = heads_g[...].astype(F32).reshape(rows, width).astype(BF16)
    tsends = {}
    for step in range(1, ntp):
        to_tp = lax.rem(tp + step, ntp)
        halves[step - 1] = dot32(all_heads, wout[:, block_of(to_tp)]).astype(BF16)
        tsends[step] = send(halves.at[step - 1], halfr.at[step - 1], 5, step)
    mixed = dot32(all_heads, wout[:, block_of(tp)]).astype(BF16).astype(F32)
    for step in range(1, ntp):
        tsends[step].wait()
        mixed = mixed + halfr[step - 1].astype(F32)
    gath3[me] = (gath2[me].astype(F32) + mixed).astype(BF16)
    copies = spread(gath3, 6)
    last = half_block(gath3, copies, gain2, wg2, wu2, wd2, part2, recv2, 7)
    out_v[...] = (gath3[me].astype(F32) + 0.5 * last).astype(BF16)
    out_copy = pltpu.make_async_copy(out_v, out_h, out_sem.at[1])
    out_copy.start()
    out_copy.wait()
    state_copy.wait()


def shards(*args):
    nkv, ntp = lax.axis_size("kv"), lax.axis_size("tp")
    n = nkv * ntp
    tokens, state, strength = args[0], args[16], args[10]
    rows, cols = tokens.shape
    seqs, heads, hd, _ = state.shape
    if cols % 128 or ntp < 2 or nkv < 2 or 2 * seqs * heads > hd or seqs % 8:
        return shards_plain(*args)
    args = [a.reshape(1, -1) if a.ndim == 1 else a for a in args]
    width = heads * hd
    buffers = [pltpu.VMEM(a.shape, a.dtype) for a in args[1:]]
    buffers += [pltpu.VMEM((n, rows, cols), BF16)] * 3
    buffers += [pltpu.VMEM((n - 1, rows, cols), BF16)] * 4
    buffers += [
        pltpu.VMEM((nkv, seqs, 4 * width), BF16),
        pltpu.VMEM((nkv - 1, seqs, 4 * width), BF16),
        pltpu.VMEM((nkv, seqs, width), BF16),
        pltpu.VMEM((ntp - 1, rows, cols), BF16),
        pltpu.VMEM((ntp - 1, rows, cols), BF16),
        pltpu.VMEM((3, rows, 128), F32),
        pltpu.VMEM((heads, seqs, hd), F32),
        pltpu.VMEM((heads, seqs, hd), F32),
        pltpu.VMEM(state.shape, F32),
        pltpu.VMEM((rows, cols), BF16),
        pltpu.SemaphoreType.DMA((len(args),)),
        pltpu.SemaphoreType.DMA((2,)),
        pltpu.SemaphoreType.DMA((8, n)),
        pltpu.SemaphoreType.DMA((8, n)),
    ]
    return pl.pallas_call(
        functools.partial(layer_kernel, nkv, ntp),
        out_shape=(
            jax.ShapeDtypeStruct(tokens.shape, tokens.dtype),
            jax.ShapeDtypeStruct(state.shape, state.dtype),
        ),
        in_specs=[pl.BlockSpec(memory_space=pl.ANY)] * len(args),
        out_specs=[pl.BlockSpec(memory_space=pl.ANY)] * 2,
        scratch_shapes=buffers,
        compiler_params=pltpu.CompilerParams(
            collective_id=0, has_side_effects=True, vmem_limit_bytes=60 * 1024 * 1024
        ),
    )(*args)


def solution(mesh):
    placed = (
        P("dp", ("kv", "tp")),
        P(),
        P(None, ("kv", "tp")),
        P(None, ("kv", "tp")),
        P(("kv", "tp"), None),
        P(),
        P("kv", "tp"),
        P("kv", "tp"),
        P("kv", "tp"),
        P("kv", "tp"),
        P(),
        P(),
        P(),
        P(),
        P(("dp", "kv"), "tp"),
        P(),
        P(("dp", "kv"), "tp", None, None),
        P("tp", "kv"),
        P(),
        P(None, ("kv", "tp")),
        P(None, ("kv", "tp")),
        P(("kv", "tp"), None),
    )
    return jax.shard_map(
        shards,
        mesh=mesh,
        in_specs=placed,
        out_specs=(P("dp", ("kv", "tp")), P(("dp", "kv"), "tp", None, None)),
        check_vma=False,
    )
```

```python
import functools

import jax
import jax.numpy as jnp
from jax import lax
from jax.experimental import pallas as pl
from jax.experimental.pallas import tpu as pltpu
from jax.sharding import PartitionSpec as P

EPS = 1e-06


def row_scale(values):
    return lax.rsqrt(jnp.mean(values * values, axis=-1, keepdims=True) + EPS)


def unit_rows(values):
    return values * lax.rsqrt(jnp.sum(values * values, axis=-1, keepdims=True) + EPS)


def block_terms(row_data, gain_vec, w_gate, w_up, w_down):
    rows32 = row_data.astype(jnp.float32)
    normed = (rows32 * row_scale(rows32) * gain_vec).astype(jnp.bfloat16)
    gate_pre = jnp.dot(normed, w_gate, preferred_element_type=jnp.float32)
    upward = jnp.dot(normed, w_up, preferred_element_type=jnp.float32)
    hidden = (jax.nn.silu(gate_pre) * upward).astype(jnp.bfloat16)
    return jnp.dot(hidden, w_down, preferred_element_type=jnp.float32)


def delta_step(
    query_vec, key_vec, value_vec, gate_vals, beta_gate, head_decay_rate, state, head_norm_gain
):
    recalled = jnp.einsum("shd,shde->she", key_vec, state, precision=lax.Precision.HIGHEST)
    correction = beta_gate[..., None] * (value_vec - head_decay_rate[..., None] * recalled)
    new_state = (
        head_decay_rate[..., None, None] * state + key_vec[..., :, None] * correction[..., None, :]
    )
    read_out = jnp.einsum("shd,shde->she", query_vec, new_state, precision=lax.Precision.HIGHEST)
    normed = read_out * row_scale(read_out) * head_norm_gain
    return (normed * jax.nn.silu(gate_vals), new_state)


def shards_plain(
    tokens,
    first_norm_gain,
    first_gate_weight,
    first_up_weight,
    first_down_weight,
    mixer_norm_gain,
    query_weight,
    key_weight,
    value_weight,
    output_gate_weight,
    strength_weight,
    decay_weight,
    head_decay_log,
    decay_input_bias,
    decay_extra_log,
    head_norm_gain,
    state,
    mixer_output_weight,
    second_norm_gain,
    second_gate_weight,
    second_up_weight,
    second_down_weight,
):
    batch_rows, columns = tokens.shape
    kv_index = lax.axis_index("kv")
    tp_index = lax.axis_index("tp")
    own_block = kv_index * lax.axis_size("tp") + tp_index
    seq_dev, heads_dev, head_size = (state.shape[0], state.shape[1], state.shape[2])
    kv_width = query_weight.shape[0]
    head_cols = heads_dev * head_size
    model_width = mixer_norm_gain.shape[0]
    rows_all = lax.all_gather(tokens, ("kv", "tp"), axis=1, tiled=True)
    ffn_terms = block_terms(
        rows_all, first_norm_gain, first_gate_weight, first_up_weight, first_down_weight
    )
    share_sum = lax.psum_scatter(
        ffn_terms.astype(jnp.bfloat16), ("kv", "tp"), scatter_dimension=1, tiled=True
    ).astype(jnp.float32)
    first_rows = (tokens.astype(jnp.float32) + 0.5 * share_sum).astype(jnp.bfloat16)
    first32 = first_rows.astype(jnp.float32)
    kv_block = lax.all_gather(first_rows, "tp", axis=1, tiled=True)
    own_gain = lax.dynamic_slice_in_dim(mixer_norm_gain, own_block * columns, columns)
    own_scaled = (first32 * own_gain).astype(jnp.bfloat16)
    beta_rows = lax.dynamic_slice_in_dim(strength_weight, own_block * columns, columns, 0)
    decay_rows = lax.dynamic_slice_in_dim(decay_weight, own_block * columns, columns, 0)
    squares, beta_pre, decay_logits = lax.psum(
        (
            jnp.sum(first32 * first32, axis=1),
            jnp.dot(own_scaled, beta_rows, preferred_element_type=jnp.float32),
            jnp.dot(own_scaled, decay_rows, preferred_element_type=jnp.float32),
        ),
        ("kv", "tp"),
    )
    row_factor = lax.rsqrt(squares / model_width + EPS)
    block_gain = lax.dynamic_slice_in_dim(mixer_norm_gain, kv_index * kv_width, kv_width)
    block_scaled = (kv_block.astype(jnp.float32) * block_gain).astype(jnp.bfloat16)
    projected = lax.psum_scatter(
        jnp.concatenate(
            [
                jnp.dot(block_scaled, weight, preferred_element_type=jnp.float32)
                for weight in (query_weight, key_weight, value_weight, output_gate_weight)
            ],
            axis=1,
        ).astype(jnp.bfloat16),
        "kv",
        scatter_dimension=0,
        tiled=True,
    ).astype(jnp.float32)
    own_rows = kv_index * seq_dev
    own_factor = lax.dynamic_slice_in_dim(row_factor, own_rows, seq_dev)[:, None]
    projected = projected * own_factor

    def split_heads(role_index):
        return projected[:, role_index * head_cols : (role_index + 1) * head_cols].reshape(
            seq_dev, heads_dev, head_size
        )

    query_vec = unit_rows(jax.nn.silu(split_heads(0))) * head_size ** (-0.5)
    key_vec = unit_rows(jax.nn.silu(split_heads(1)))
    value_vec = jax.nn.silu(split_heads(2))
    gate_vals = split_heads(3)
    head_start = tp_index * heads_dev

    def local_gate_values(values):
        own_seqs = lax.dynamic_slice_in_dim(values, own_rows, seq_dev, 0)
        return lax.dynamic_slice_in_dim(own_seqs, head_start, heads_dev, 1) * own_factor

    beta_gate = jax.nn.sigmoid(local_gate_values(beta_pre))
    decay_log_term = lax.dynamic_slice_in_dim(head_decay_log, head_start, heads_dev)
    decay_offset_term = lax.dynamic_slice_in_dim(decay_input_bias, head_start, heads_dev)
    head_decay_rate = jnp.exp(
        decay_extra_log
        - jnp.exp(decay_log_term)
        * jax.nn.softplus(local_gate_values(decay_logits) + decay_offset_term)
    )
    heads_f32, new_state = delta_step(
        query_vec, key_vec, value_vec, gate_vals, beta_gate, head_decay_rate, state, head_norm_gain
    )
    heads_out = heads_f32.reshape(seq_dev, head_cols).astype(jnp.bfloat16)
    mixer_terms = jnp.dot(
        lax.all_gather(heads_out, "kv", axis=0, tiled=True),
        mixer_output_weight,
        preferred_element_type=jnp.float32,
    )
    mixer_sum = lax.psum_scatter(
        mixer_terms.astype(jnp.bfloat16), "tp", scatter_dimension=1, tiled=True
    ).astype(jnp.float32)
    second_rows = (first32 + mixer_sum).astype(jnp.bfloat16)
    rows_last = lax.all_gather(second_rows, ("kv", "tp"), axis=1, tiled=True)
    last_terms = block_terms(
        rows_last, second_norm_gain, second_gate_weight, second_up_weight, second_down_weight
    )
    last_sum = lax.psum_scatter(
        last_terms.astype(jnp.bfloat16), ("kv", "tp"), scatter_dimension=1, tiled=True
    ).astype(jnp.float32)
    layer_out = (second_rows.astype(jnp.float32) + 0.5 * last_sum).astype(jnp.bfloat16)
    return (layer_out, new_state)


MESH = pl.DeviceIdType.MESH
BF16 = jnp.bfloat16
F32 = jnp.float32


def dot32(a, b):
    return jnp.dot(a, b, preferred_element_type=F32)


def dot32t(a, b):
    return lax.dot_general(a, b, (((1,), (1,)), ((), ())), preferred_element_type=F32)


def silu(x):
    return x * jax.nn.sigmoid(x)


def layer_kernel(nkv, ntp, *refs):
    (tok_h, gain1_h, wg1_h, wu1_h, wd1_h, mgain_h, wq_h, wk_h, wv_h, wo_h, ws_h, wdec_h,
     hlog_h, bias_h, extra_h, hgain_h, state_h, wout_h, gain2_h, wg2_h, wu2_h, wd2_h,
     out_h, new_h,
     gain1, wg1, wu1, wd1, mgain, wq, wk, wv, wo, ws, wdec, hlog, bias, extra, hgain,
     state, wout, gain2, wg2, wu2, wd2,
     gath1, gath2, gath3, part1, recv1, part2, recv2, projs, projr, heads_g, halves, halfr,
     stat, statr, split, ks_v, qs_v, newst, out_v, load_sem, out_sem, send_sem, recv_sem) = refs
    n = nkv * ntp
    kv = lax.axis_index("kv")
    tp = lax.axis_index("tp")
    me = kv * ntp + tp
    rows, cols = tok_h.shape
    seqs, heads, hd, _ = state_h.shape
    width = heads * hd
    model = n * cols

    tok_copy = pltpu.make_async_copy(tok_h, gath1.at[me], load_sem.at[0])
    tok_copy.start()
    order = [(gain1_h, gain1), (wg1_h, wg1), (wu1_h, wu1), (wd1_h, wd1), (mgain_h, mgain),
             (wq_h, wq), (wk_h, wk), (wv_h, wv), (wo_h, wo), (ws_h, ws), (wdec_h, wdec),
             (hlog_h, hlog), (bias_h, bias), (extra_h, extra), (hgain_h, hgain),
             (state_h, state), (wout_h, wout), (gain2_h, gain2), (wg2_h, wg2),
             (wu2_h, wu2), (wd2_h, wd2)]
    loads = {}

    def fetch(start, stop):
        for at in range(start, stop):
            source, dest = order[at]
            copy = pltpu.make_async_copy(source, dest, load_sem.at[at + 1])
            copy.start()
            loads[id(dest)] = copy

    fetch(0, 4)

    def need(*dests):
        for dest in dests:
            loads[id(dest)].wait()

    def peer(step):
        to_kv = lax.rem(kv + step // ntp, nkv)
        to_tp = lax.rem(tp + step % ntp, ntp)
        return to_kv * ntp + to_tp, {"kv": to_kv, "tp": to_tp}

    def origin(step):
        return lax.rem(kv + nkv - step // ntp, nkv) * ntp + lax.rem(tp + ntp - step % ntp, ntp)

    barrier = pltpu.get_barrier_semaphore()
    for step in range(1, n):
        pl.semaphore_signal(barrier, inc=1, device_id=peer(step)[1], device_id_type=MESH)
    pl.semaphore_wait(barrier, n - 1)

    def send(source, dest, phase, step):
        copy = pltpu.make_async_remote_copy(
            src_ref=source, dst_ref=dest, send_sem=send_sem.at[phase, step],
            recv_sem=recv_sem.at[phase, step], device_id=peer(step)[1], device_id_type=MESH)
        copy.start()
        return copy

    def spread(gath, phase, stop=n):
        return {step: send(gath.at[me], gath.at[me], phase, step) for step in range(1, stop)}

    def block_of(at):
        return pl.ds(pl.multiple_of(at * cols, cols), cols)

    def half_block(gath, copies, gain, w_gate, w_up, w_down, part, recv, phase, then):
        def take(source, carry):
            squares, gate, up = carry
            block = gath[source].astype(F32)
            squares = squares + jnp.sum(block * block, axis=1, keepdims=True)
            scaled = (block * gain[:, block_of(source)]).astype(BF16)
            gate = gate + dot32t(scaled, w_gate[:, block_of(source)])
            up = up + dot32t(scaled, w_up[:, block_of(source)])
            return (squares, gate, up)

        hidden_cols = w_gate.shape[0]
        need(gain, w_gate, w_up)
        fetch(*then)
        zeros = jnp.zeros((rows, hidden_cols), F32)
        carry = take(me, (jnp.zeros((rows, 1), F32), zeros, zeros))
        for step in range(1, n):
            copies[step].wait()
            carry = take(origin(step), carry)
        squares, gate, up = carry
        factor = lax.rsqrt(squares / model + EPS)
        hidden = (silu(gate * factor) * (up * factor)).astype(BF16)
        need(w_down)
        sends = {}
        for step in range(1, n):
            part[step - 1] = dot32(hidden, w_down[:, block_of(peer(step)[0])]).astype(BF16)
            sends[step] = send(part.at[step - 1], recv.at[step - 1], phase, step)
        total = dot32(hidden, w_down[:, block_of(me)])
        for step in range(1, n):
            sends[step].wait()
            total = total + recv[step - 1].astype(F32)
        return total

    tok_copy.wait()
    copies = spread(gath1, 0)
    share = half_block(gath1, copies, gain1, wg1, wu1, wd1, part1, recv1, 1, (4, 17))
    first = (gath1[me].astype(F32) + 0.5 * share).astype(BF16)
    gath2[me] = first
    copies = spread(gath2, 2, ntp)
    fetch(17, len(order))

    def scaled_block(source):
        return (gath2[source].astype(F32) * mgain[:, block_of(source)]).astype(BF16)

    need(mgain, ws, wdec, hlog, bias, extra, hgain)
    all_heads = ws.shape[0]
    first32 = first.astype(F32)
    scaled = scaled_block(me)
    stat[...] = jnp.zeros_like(stat)
    for at, values in (
        (0, dot32t(scaled, ws[:, block_of(me)])),
        (all_heads, dot32t(scaled, wdec[:, block_of(me)])),
        (2 * all_heads, jnp.sum(first32 * first32, axis=1, keepdims=True)),
    ):
        lanes = values.shape[1]
        stat[:, :, at:at + lanes] = values.reshape(nkv, seqs, lanes)
    ssends = {}
    for step in range(1, n):
        ssends[step] = send(stat.at[peer(step)[0] // ntp], statr.at[step - 1], 8, step)

    need(wq, wk, wv, wo)
    acc = [jnp.zeros((rows, width), F32) for _ in range(4)]
    for step in range(ntp):
        if step:
            copies[step].wait()
        source = origin(step)
        local = block_of(lax.rem(source, ntp))
        scaled = scaled_block(source)
        acc = [a + dot32(scaled, w[local, :]) for a, w in zip(acc, (wq, wk, wv, wo))]
    for role in range(4):
        projs[:, :, role * width:(role + 1) * width] = acc[role].reshape(nkv, seqs, width).astype(BF16)
    psends = {}
    for dk in range(1, nkv):
        to_kv = lax.rem(kv + dk, nkv)
        psends[dk] = send(projs.at[to_kv], projr.at[dk - 1], 3, dk * ntp)

    need(state)
    for h in range(heads):
        for s in range(seqs):
            mat = state[s, h]
            high = mat.astype(BF16)
            beside = slice((s % 2) * hd, (s % 2 + 1) * hd)
            split[h, s // 2, 0:hd, beside] = high
            split[h, s // 2, hd:2 * hd, beside] = (mat - high.astype(F32)).astype(BF16)

    totals = stat[kv]
    for step in range(1, n):
        ssends[step].wait()
        totals = totals + statr[step - 1]
    factor = lax.rsqrt(totals[:, 2 * all_heads:2 * all_heads + 1] / model + EPS)

    def own_heads(values):
        picked = values[:, 0:heads]
        for at in range(1, ntp):
            picked = jnp.where(tp == at, values[:, at * heads:(at + 1) * heads], picked)
        return picked

    beta = jax.nn.sigmoid(own_heads(totals) * factor)
    logits = own_heads(totals[:, all_heads:2 * all_heads]) * factor + own_heads(bias[...])
    softplus = jnp.maximum(logits, 0.0) + jnp.log1p(jnp.exp(-jnp.abs(logits)))
    decay = jnp.exp(extra[...].T - jnp.exp(own_heads(hlog[...])) * softplus)

    summed = projs[kv].astype(F32)
    for dk in range(1, nkv):
        psends[dk].wait()
        summed = summed + projr[dk - 1].astype(F32)
    summed = summed * factor

    def role_head(role, h):
        start = role * width + h * hd
        return summed[:, start:start + hd]

    def unit(u):
        return u * lax.rsqrt(jnp.sum(u * u, axis=-1, keepdims=True) + EPS)

    key_h = [unit(silu(role_head(1, h))) for h in range(heads)]
    query_hs = [unit(silu(role_head(0, h))) * hd ** (-0.5) for h in range(heads)]
    row_at = lax.broadcasted_iota(jnp.int32, (seqs, hd), 0)
    recalled = []
    asked = []
    for h in range(heads):
        both = jnp.concatenate([key_h[h], query_hs[h]], axis=0)
        high = both.astype(BF16).astype(F32)
        terms = jnp.concatenate([high, both - high], axis=0).astype(BF16)
        terms = jnp.concatenate([terms, terms], axis=1)
        sums = [jnp.zeros((seqs, hd), F32)] * 2
        for half in range(seqs // 2):
            found = dot32(terms, split[h, half])
            found = found[0:2 * seqs] + found[2 * seqs:4 * seqs]
            for s in (0, 1):
                own_row = row_at == 2 * half + s
                for role in (0, 1):
                    part = found[role * seqs:(role + 1) * seqs, s * hd:(s + 1) * hd]
                    sums[role] = jnp.where(own_row, part, sums[role])
        recalled.append(sums[0])
        asked.append(sums[1])
    corrections = []
    decays = []
    outs = []
    for h in range(heads):
        rate = jnp.broadcast_to(decay[:, h:h + 1], (seqs, hd))
        correction = beta[:, h:h + 1] * (silu(role_head(2, h)) - rate * recalled[h])
        mix = jnp.sum(query_hs[h] * key_h[h], axis=1, keepdims=True)
        read = rate * asked[h] + mix * correction
        normed = read * lax.rsqrt(jnp.mean(read * read, axis=-1, keepdims=True) + EPS) * hgain[...]
        outs.append((normed * silu(role_head(3, h))).astype(BF16))
        corrections.append(correction)
        decays.append(rate)
    for h in range(heads):
        heads_g[kv, :, h * hd:(h + 1) * hd] = outs[h]
    hsends = {dk: send(heads_g.at[kv], heads_g.at[kv], 4, dk * ntp) for dk in range(1, nkv)}

    pad = jnp.zeros((hd - heads * seqs, hd), F32)
    turned = jnp.concatenate(key_h + [pad], axis=0).T
    for h in range(heads):
        ks_v[h] = corrections[h]
        qs_v[h] = decays[h]
    for h in range(heads):
        for s in range(seqs):
            at = h * seqs + s
            newst[s, h] = qs_v[h, s:s + 1, :] * state[s, h] + turned[:, at:at + 1] * ks_v[h, s:s + 1, :]
    state_copy = pltpu.make_async_copy(newst, new_h, out_sem.at[0])
    state_copy.start()

    need(wout)
    for dk in range(1, nkv):
        hsends[dk].wait()
    gathered = heads_g[...].astype(F32).reshape(rows, width).astype(BF16)
    tsends = {}
    for step in range(1, ntp):
        to_tp = lax.rem(tp + step, ntp)
        halves[step - 1] = dot32(gathered, wout[:, block_of(to_tp)]).astype(BF16)
        tsends[step] = send(halves.at[step - 1], halfr.at[step - 1], 5, step)
    mixed = dot32(gathered, wout[:, block_of(tp)]).astype(BF16).astype(F32)
    for step in range(1, ntp):
        tsends[step].wait()
        mixed = mixed + halfr[step - 1].astype(F32)
    gath3[me] = (gath2[me].astype(F32) + mixed).astype(BF16)
    copies = spread(gath3, 6)
    last = half_block(gath3, copies, gain2, wg2, wu2, wd2, part2, recv2, 7, (0, 0))
    out_v[...] = (gath3[me].astype(F32) + 0.5 * last).astype(BF16)
    out_copy = pltpu.make_async_copy(out_v, out_h, out_sem.at[1])
    out_copy.start()
    out_copy.wait()
    state_copy.wait()


def shards(*args):
    nkv, ntp = lax.axis_size("kv"), lax.axis_size("tp")
    n = nkv * ntp
    tokens, state, strength = args[0], args[16], args[10]
    rows, cols = tokens.shape
    seqs, heads, hd, _ = state.shape
    if cols % 128 or ntp < 2 or nkv < 2 or seqs * heads > hd or seqs % 8:
        return shards_plain(*args)
    args = [a.reshape(1, -1) if a.ndim == 1 else a for a in args]
    for at in (2, 3, 10, 11, 14, 19, 20):
        args[at] = args[at].T
    width = heads * hd
    buffers = [pltpu.VMEM(a.shape, a.dtype) for a in args[1:]]
    buffers += [pltpu.VMEM((n, rows, cols), BF16)] * 3
    buffers += [pltpu.VMEM((n - 1, rows, cols), BF16)] * 4
    buffers += [
        pltpu.VMEM((nkv, seqs, 4 * width), BF16),
        pltpu.VMEM((nkv - 1, seqs, 4 * width), BF16),
        pltpu.VMEM((nkv, seqs, width), BF16),
        pltpu.VMEM((ntp - 1, rows, cols), BF16),
        pltpu.VMEM((ntp - 1, rows, cols), BF16),
        pltpu.VMEM((nkv, seqs, 128), F32),
        pltpu.VMEM((n - 1, seqs, 128), F32),
        pltpu.VMEM((heads, seqs // 2, 2 * hd, 2 * hd), BF16),
        pltpu.VMEM((heads, seqs, hd), F32),
        pltpu.VMEM((heads, seqs, hd), F32),
        pltpu.VMEM(state.shape, F32),
        pltpu.VMEM((rows, cols), BF16),
        pltpu.SemaphoreType.DMA((len(args),)),
        pltpu.SemaphoreType.DMA((2,)),
        pltpu.SemaphoreType.DMA((9, n)),
        pltpu.SemaphoreType.DMA((9, n)),
    ]
    return pl.pallas_call(
        functools.partial(layer_kernel, nkv, ntp),
        out_shape=(
            jax.ShapeDtypeStruct(tokens.shape, tokens.dtype),
            jax.ShapeDtypeStruct(state.shape, state.dtype),
        ),
        in_specs=[pl.BlockSpec(memory_space=pl.ANY)] * len(args),
        out_specs=[pl.BlockSpec(memory_space=pl.ANY)] * 2,
        scratch_shapes=buffers,
        compiler_params=pltpu.CompilerParams(
            collective_id=0, has_side_effects=True, vmem_limit_bytes=60 * 1024 * 1024
        ),
    )(*args)


def solution(mesh):
    placed = (
        P("dp", ("kv", "tp")),
        P(),
        P(None, ("kv", "tp")),
        P(None, ("kv", "tp")),
        P(("kv", "tp"), None),
        P(),
        P("kv", "tp"),
        P("kv", "tp"),
        P("kv", "tp"),
        P("kv", "tp"),
        P(),
        P(),
        P(),
        P(),
        P(("dp", "kv"), "tp"),
        P(),
        P(("dp", "kv"), "tp", None, None),
        P("tp", "kv"),
        P(),
        P(None, ("kv", "tp")),
        P(None, ("kv", "tp")),
        P(("kv", "tp"), None),
    )
    return jax.shard_map(
        shards,
        mesh=mesh,
        in_specs=placed,
        out_specs=(P("dp", ("kv", "tp")), P(("dp", "kv"), "tp", None, None)),
        check_vma=False,
    )
```

```python
import functools

import jax
import jax.numpy as jnp
from jax import lax
from jax.experimental import pallas as pl
from jax.experimental.pallas import tpu as pltpu
from jax.sharding import PartitionSpec as P

EPS = 1e-06


def row_scale(values):
    return lax.rsqrt(jnp.mean(values * values, axis=-1, keepdims=True) + EPS)


def unit_rows(values):
    return values * lax.rsqrt(jnp.sum(values * values, axis=-1, keepdims=True) + EPS)


def block_terms(row_data, gain_vec, w_gate, w_up, w_down):
    rows32 = row_data.astype(jnp.float32)
    normed = (rows32 * row_scale(rows32) * gain_vec).astype(jnp.bfloat16)
    gate_pre = jnp.dot(normed, w_gate, preferred_element_type=jnp.float32)
    upward = jnp.dot(normed, w_up, preferred_element_type=jnp.float32)
    hidden = (jax.nn.silu(gate_pre) * upward).astype(jnp.bfloat16)
    return jnp.dot(hidden, w_down, preferred_element_type=jnp.float32)


def delta_step(
    query_vec, key_vec, value_vec, gate_vals, beta_gate, head_decay_rate, state, head_norm_gain
):
    recalled = jnp.einsum("shd,shde->she", key_vec, state, precision=lax.Precision.HIGHEST)
    correction = beta_gate[..., None] * (value_vec - head_decay_rate[..., None] * recalled)
    new_state = (
        head_decay_rate[..., None, None] * state + key_vec[..., :, None] * correction[..., None, :]
    )
    read_out = jnp.einsum("shd,shde->she", query_vec, new_state, precision=lax.Precision.HIGHEST)
    normed = read_out * row_scale(read_out) * head_norm_gain
    return (normed * jax.nn.silu(gate_vals), new_state)


def shards_plain(
    tokens,
    first_norm_gain,
    first_gate_weight,
    first_up_weight,
    first_down_weight,
    mixer_norm_gain,
    query_weight,
    key_weight,
    value_weight,
    output_gate_weight,
    strength_weight,
    decay_weight,
    head_decay_log,
    decay_input_bias,
    decay_extra_log,
    head_norm_gain,
    state,
    mixer_output_weight,
    second_norm_gain,
    second_gate_weight,
    second_up_weight,
    second_down_weight,
):
    batch_rows, columns = tokens.shape
    kv_index = lax.axis_index("kv")
    tp_index = lax.axis_index("tp")
    own_block = kv_index * lax.axis_size("tp") + tp_index
    seq_dev, heads_dev, head_size = (state.shape[0], state.shape[1], state.shape[2])
    kv_width = query_weight.shape[0]
    head_cols = heads_dev * head_size
    model_width = mixer_norm_gain.shape[0]
    rows_all = lax.all_gather(tokens, ("kv", "tp"), axis=1, tiled=True)
    ffn_terms = block_terms(
        rows_all, first_norm_gain, first_gate_weight, first_up_weight, first_down_weight
    )
    share_sum = lax.psum_scatter(
        ffn_terms.astype(jnp.bfloat16), ("kv", "tp"), scatter_dimension=1, tiled=True
    ).astype(jnp.float32)
    first_rows = (tokens.astype(jnp.float32) + 0.5 * share_sum).astype(jnp.bfloat16)
    first32 = first_rows.astype(jnp.float32)
    kv_block = lax.all_gather(first_rows, "tp", axis=1, tiled=True)
    own_gain = lax.dynamic_slice_in_dim(mixer_norm_gain, own_block * columns, columns)
    own_scaled = (first32 * own_gain).astype(jnp.bfloat16)
    beta_rows = lax.dynamic_slice_in_dim(strength_weight, own_block * columns, columns, 0)
    decay_rows = lax.dynamic_slice_in_dim(decay_weight, own_block * columns, columns, 0)
    squares, beta_pre, decay_logits = lax.psum(
        (
            jnp.sum(first32 * first32, axis=1),
            jnp.dot(own_scaled, beta_rows, preferred_element_type=jnp.float32),
            jnp.dot(own_scaled, decay_rows, preferred_element_type=jnp.float32),
        ),
        ("kv", "tp"),
    )
    row_factor = lax.rsqrt(squares / model_width + EPS)
    block_gain = lax.dynamic_slice_in_dim(mixer_norm_gain, kv_index * kv_width, kv_width)
    block_scaled = (kv_block.astype(jnp.float32) * block_gain).astype(jnp.bfloat16)
    projected = lax.psum_scatter(
        jnp.concatenate(
            [
                jnp.dot(block_scaled, weight, preferred_element_type=jnp.float32)
                for weight in (query_weight, key_weight, value_weight, output_gate_weight)
            ],
            axis=1,
        ).astype(jnp.bfloat16),
        "kv",
        scatter_dimension=0,
        tiled=True,
    ).astype(jnp.float32)
    own_rows = kv_index * seq_dev
    own_factor = lax.dynamic_slice_in_dim(row_factor, own_rows, seq_dev)[:, None]
    projected = projected * own_factor

    def split_heads(role_index):
        return projected[:, role_index * head_cols : (role_index + 1) * head_cols].reshape(
            seq_dev, heads_dev, head_size
        )

    query_vec = unit_rows(jax.nn.silu(split_heads(0))) * head_size ** (-0.5)
    key_vec = unit_rows(jax.nn.silu(split_heads(1)))
    value_vec = jax.nn.silu(split_heads(2))
    gate_vals = split_heads(3)
    head_start = tp_index * heads_dev

    def local_gate_values(values):
        own_seqs = lax.dynamic_slice_in_dim(values, own_rows, seq_dev, 0)
        return lax.dynamic_slice_in_dim(own_seqs, head_start, heads_dev, 1) * own_factor

    beta_gate = jax.nn.sigmoid(local_gate_values(beta_pre))
    decay_log_term = lax.dynamic_slice_in_dim(head_decay_log, head_start, heads_dev)
    decay_offset_term = lax.dynamic_slice_in_dim(decay_input_bias, head_start, heads_dev)
    head_decay_rate = jnp.exp(
        decay_extra_log
        - jnp.exp(decay_log_term)
        * jax.nn.softplus(local_gate_values(decay_logits) + decay_offset_term)
    )
    heads_f32, new_state = delta_step(
        query_vec, key_vec, value_vec, gate_vals, beta_gate, head_decay_rate, state, head_norm_gain
    )
    heads_out = heads_f32.reshape(seq_dev, head_cols).astype(jnp.bfloat16)
    mixer_terms = jnp.dot(
        lax.all_gather(heads_out, "kv", axis=0, tiled=True),
        mixer_output_weight,
        preferred_element_type=jnp.float32,
    )
    mixer_sum = lax.psum_scatter(
        mixer_terms.astype(jnp.bfloat16), "tp", scatter_dimension=1, tiled=True
    ).astype(jnp.float32)
    second_rows = (first32 + mixer_sum).astype(jnp.bfloat16)
    rows_last = lax.all_gather(second_rows, ("kv", "tp"), axis=1, tiled=True)
    last_terms = block_terms(
        rows_last, second_norm_gain, second_gate_weight, second_up_weight, second_down_weight
    )
    last_sum = lax.psum_scatter(
        last_terms.astype(jnp.bfloat16), ("kv", "tp"), scatter_dimension=1, tiled=True
    ).astype(jnp.float32)
    layer_out = (second_rows.astype(jnp.float32) + 0.5 * last_sum).astype(jnp.bfloat16)
    return (layer_out, new_state)


MESH = pl.DeviceIdType.MESH
BF16 = jnp.bfloat16
F32 = jnp.float32


def dot32(a, b):
    return jnp.dot(a, b, preferred_element_type=F32)


def dot32t(a, b):
    return lax.dot_general(a, b, (((1,), (1,)), ((), ())), preferred_element_type=F32)


def silu(x):
    return x * jax.nn.sigmoid(x)


def layer_kernel(nkv, ntp, *refs):
    (tok_h, gain1_h, wg1_h, wu1_h, wd1_h, mgain_h, wq_h, wk_h, wv_h, wo_h, ws_h, wdec_h,
     hlog_h, bias_h, extra_h, hgain_h, state_h, wout_h, gain2_h, wg2_h, wu2_h, wd2_h,
     out_h, new_h,
     gain1, wg1, wu1, wd1, mgain, wq, wk, wv, wo, ws, wdec, hlog, bias, extra, hgain,
     state, wout, gain2, wg2, wu2, wd2,
     gath1, gath2, gath3, part1, recv1, part2, recv2, projs, projr, heads_g, halves, halfr,
     stat, statr, split, ks_v, qs_v, newst, out_v, load_sem, out_sem, send_sem, recv_sem) = refs
    n = nkv * ntp
    kv = lax.axis_index("kv")
    tp = lax.axis_index("tp")
    me = kv * ntp + tp
    rows, cols = tok_h.shape
    seqs, heads, hd, _ = state_h.shape
    width = heads * hd
    model = n * cols

    tok_copy = pltpu.make_async_copy(tok_h, gath1.at[me], load_sem.at[0])
    tok_copy.start()
    order = [(gain1_h, gain1), (wg1_h, wg1), (wu1_h, wu1), (wd1_h, wd1), (mgain_h, mgain),
             (wq_h, wq), (wk_h, wk), (wv_h, wv), (wo_h, wo), (ws_h, ws), (wdec_h, wdec),
             (hlog_h, hlog), (bias_h, bias), (extra_h, extra), (hgain_h, hgain),
             (state_h, state), (wout_h, wout), (gain2_h, gain2), (wg2_h, wg2),
             (wu2_h, wu2), (wd2_h, wd2)]
    loads = {}

    def fetch(start, stop):
        for at in range(start, stop):
            source, dest = order[at]
            copy = pltpu.make_async_copy(source, dest, load_sem.at[at + 1])
            copy.start()
            loads[id(dest)] = copy

    fetch(0, 4)

    def need(*dests):
        for dest in dests:
            loads[id(dest)].wait()

    def peer(step):
        to_kv = lax.rem(kv + step // ntp, nkv)
        to_tp = lax.rem(tp + step % ntp, ntp)
        return to_kv * ntp + to_tp, {"kv": to_kv, "tp": to_tp}

    def origin(step):
        return lax.rem(kv + nkv - step // ntp, nkv) * ntp + lax.rem(tp + ntp - step % ntp, ntp)

    barrier = pltpu.get_barrier_semaphore()
    for step in range(1, n):
        pl.semaphore_signal(barrier, inc=1, device_id=peer(step)[1], device_id_type=MESH)
    pl.semaphore_wait(barrier, n - 1)

    def send(source, dest, phase, step):
        copy = pltpu.make_async_remote_copy(
            src_ref=source, dst_ref=dest, send_sem=send_sem.at[phase, step],
            recv_sem=recv_sem.at[phase, step], device_id=peer(step)[1], device_id_type=MESH)
        copy.start()
        return copy

    def spread(gath, phase, stop=n):
        return {step: send(gath.at[me], gath.at[me], phase, step) for step in range(1, stop)}

    def block_of(at):
        return pl.ds(pl.multiple_of(at * cols, cols), cols)

    def half_block(gath, copies, gain, w_gate, w_up, w_down, part, recv, phase, then):
        def take(source, carry):
            squares, gate, up = carry
            block = gath[source].astype(F32)
            squares = squares + jnp.sum(block * block, axis=1, keepdims=True)
            scaled = (block * gain[:, block_of(source)]).astype(BF16)
            gate = gate + dot32t(scaled, w_gate[:, block_of(source)])
            up = up + dot32t(scaled, w_up[:, block_of(source)])
            return (squares, gate, up)

        hidden_cols = w_gate.shape[0]
        need(gain, w_gate, w_up)
        fetch(*then)
        zeros = jnp.zeros((rows, hidden_cols), F32)
        carry = take(me, (jnp.zeros((rows, 1), F32), zeros, zeros))
        for step in range(1, n):
            copies[step].wait()
            carry = take(origin(step), carry)
        squares, gate, up = carry
        factor = lax.rsqrt(squares / model + EPS)
        hidden = (silu(gate * factor) * (up * factor)).astype(BF16)
        need(w_down)
        sends = {}
        for step in range(1, n):
            part[step - 1] = dot32(hidden, w_down[:, block_of(peer(step)[0])]).astype(BF16)
            sends[step] = send(part.at[step - 1], recv.at[step - 1], phase, step)
        total = dot32(hidden, w_down[:, block_of(me)])
        for step in range(1, n):
            sends[step].wait()
            total = total + recv[step - 1].astype(F32)
        return total

    tok_copy.wait()
    copies = spread(gath1, 0)
    share = half_block(gath1, copies, gain1, wg1, wu1, wd1, part1, recv1, 1, (4, 17))
    first = (gath1[me].astype(F32) + 0.5 * share).astype(BF16)
    gath2[me] = first
    copies = spread(gath2, 2, ntp)
    fetch(17, len(order))

    def scaled_block(source):
        return (gath2[source].astype(F32) * mgain[:, block_of(source)]).astype(BF16)

    need(mgain, ws, wdec, hlog, bias, extra, hgain)
    all_heads = ws.shape[0]
    first32 = first.astype(F32)
    scaled = scaled_block(me)
    stat[...] = jnp.zeros_like(stat)
    for at, values in (
        (0, dot32t(scaled, ws[:, block_of(me)])),
        (all_heads, dot32t(scaled, wdec[:, block_of(me)])),
        (2 * all_heads, jnp.sum(first32 * first32, axis=1, keepdims=True)),
    ):
        lanes = values.shape[1]
        stat[:, :, at:at + lanes] = values.reshape(nkv, seqs, lanes)
    ssends = {}
    for step in range(1, n):
        ssends[step] = send(stat.at[peer(step)[0] // ntp], statr.at[step - 1], 8, step)

    need(wq, wk, wv, wo)
    acc = [jnp.zeros((rows, width), F32) for _ in range(4)]
    for step in range(ntp):
        if step:
            copies[step].wait()
        source = origin(step)
        local = block_of(lax.rem(source, ntp))
        scaled = scaled_block(source)
        acc = [a + dot32(scaled, w[local, :]) for a, w in zip(acc, (wq, wk, wv, wo))]
    for role in range(4):
        projs[:, :, role * width:(role + 1) * width] = acc[role].reshape(nkv, seqs, width).astype(BF16)
    psends = {}
    for dk in range(1, nkv):
        to_kv = lax.rem(kv + dk, nkv)
        psends[dk] = send(projs.at[to_kv], projr.at[dk - 1], 3, dk * ntp)

    need(state)
    for h in range(heads):
        for s in range(seqs):
            mat = state[s, h]
            high = mat.astype(BF16)
            beside = slice((s % 2) * hd, (s % 2 + 1) * hd)
            split[h, s // 2, 0:hd, beside] = high
            split[h, s // 2, hd:2 * hd, beside] = (mat - high.astype(F32)).astype(BF16)

    totals = stat[kv]
    for step in range(1, n):
        ssends[step].wait()
        totals = totals + statr[step - 1]
    factor = lax.rsqrt(totals[:, 2 * all_heads:2 * all_heads + 1] / model + EPS)

    def own_heads(values):
        picked = values[:, 0:heads]
        for at in range(1, ntp):
            picked = jnp.where(tp == at, values[:, at * heads:(at + 1) * heads], picked)
        return picked

    beta = jax.nn.sigmoid(own_heads(totals) * factor)
    logits = own_heads(totals[:, all_heads:2 * all_heads]) * factor + own_heads(bias[...])
    softplus = jnp.maximum(logits, 0.0) + jnp.log1p(jnp.exp(-jnp.abs(logits)))
    decay = jnp.exp(extra[...].T - jnp.exp(own_heads(hlog[...])) * softplus)

    summed = projs[kv].astype(F32)
    for dk in range(1, nkv):
        psends[dk].wait()
        summed = summed + projr[dk - 1].astype(F32)
    summed = summed * factor

    def role_head(role, h):
        start = role * width + h * hd
        return summed[:, start:start + hd]

    def unit(u):
        return u * lax.rsqrt(jnp.sum(u * u, axis=-1, keepdims=True) + EPS)

    key_h = [unit(silu(role_head(1, h))) for h in range(heads)]
    query_hs = [unit(silu(role_head(0, h))) * hd ** (-0.5) for h in range(heads)]
    row_at = lax.broadcasted_iota(jnp.int32, (seqs, hd), 0)
    recalled = []
    asked = []
    for h in range(heads):
        both = jnp.concatenate([key_h[h], query_hs[h]], axis=0)
        high = both.astype(BF16).astype(F32)
        terms = jnp.concatenate([high, both - high], axis=0).astype(BF16)
        terms = jnp.concatenate([terms, terms], axis=1)
        sums = [jnp.zeros((seqs, hd), F32)] * 2
        for half in range(seqs // 2):
            found = dot32(terms, split[h, half])
            found = found[0:2 * seqs] + found[2 * seqs:4 * seqs]
            for s in (0, 1):
                own_row = row_at == 2 * half + s
                for role in (0, 1):
                    part = found[role * seqs:(role + 1) * seqs, s * hd:(s + 1) * hd]
                    sums[role] = jnp.where(own_row, part, sums[role])
        recalled.append(sums[0])
        asked.append(sums[1])
    corrections = []
    decays = []
    outs = []
    for h in range(heads):
        rate = jnp.broadcast_to(decay[:, h:h + 1], (seqs, hd))
        correction = beta[:, h:h + 1] * (silu(role_head(2, h)) - rate * recalled[h])
        mix = jnp.sum(query_hs[h] * key_h[h], axis=1, keepdims=True)
        read = rate * asked[h] + mix * correction
        normed = read * lax.rsqrt(jnp.mean(read * read, axis=-1, keepdims=True) + EPS) * hgain[...]
        outs.append((normed * silu(role_head(3, h))).astype(BF16))
        corrections.append(correction)
        decays.append(rate)
    for h in range(heads):
        heads_g[kv, :, h * hd:(h + 1) * hd] = outs[h]
    hsends = {dk: send(heads_g.at[kv], heads_g.at[kv], 4, dk * ntp) for dk in range(1, nkv)}

    pad = jnp.zeros((hd - heads * seqs, hd), F32)
    turned = jnp.concatenate(key_h + [pad], axis=0).T
    for h in range(heads):
        ks_v[h] = corrections[h]
        qs_v[h] = decays[h]
    for h in range(heads):
        for s in range(seqs):
            at = h * seqs + s
            newst[s, h] = qs_v[h, s:s + 1, :] * state[s, h] + turned[:, at:at + 1] * ks_v[h, s:s + 1, :]
    state_copy = pltpu.make_async_copy(newst, new_h, out_sem.at[0])
    state_copy.start()

    need(wout)
    for dk in range(1, nkv):
        hsends[dk].wait()
    gathered = heads_g[...].astype(F32).reshape(rows, width).astype(BF16)
    tsends = {}
    for step in range(1, ntp):
        to_tp = lax.rem(tp + step, ntp)
        halves[step - 1] = dot32(gathered, wout[:, block_of(to_tp)]).astype(BF16)
        tsends[step] = send(halves.at[step - 1], halfr.at[step - 1], 5, step)
    mixed = dot32(gathered, wout[:, block_of(tp)]).astype(BF16).astype(F32)
    for step in range(1, ntp):
        tsends[step].wait()
        mixed = mixed + halfr[step - 1].astype(F32)
    gath3[me] = (gath2[me].astype(F32) + mixed).astype(BF16)
    copies = spread(gath3, 6)
    last = half_block(gath3, copies, gain2, wg2, wu2, wd2, part2, recv2, 7, (0, 0))
    out_v[...] = (gath3[me].astype(F32) + 0.5 * last).astype(BF16)
    out_copy = pltpu.make_async_copy(out_v, out_h, out_sem.at[1])
    out_copy.start()
    out_copy.wait()
    state_copy.wait()


def hand_over(rows_h, state_h, rows_o, state_o, rows_v, state_v, in_sem, out_sem):
    count = in_sem.shape[0] - 1
    size = state_h.shape[0] // count
    spans = [pl.ds(at * size, size) for at in range(count)]
    ins = [pltpu.make_async_copy(state_h.at[span], state_v.at[span], in_sem.at[at])
           for at, span in enumerate(spans)]
    outs = [pltpu.make_async_copy(state_v.at[span], state_o.at[span], out_sem.at[at])
            for at, span in enumerate(spans)]
    ins.append(pltpu.make_async_copy(rows_h, rows_v, in_sem.at[count]))
    outs.append(pltpu.make_async_copy(rows_v, rows_o, out_sem.at[count]))
    for copy in ins:
        copy.start()
    for arrived, copy in zip(ins, outs):
        arrived.wait()
        copy.start()
    for copy in outs:
        copy.wait()


def shards(*args):
    nkv, ntp = lax.axis_size("kv"), lax.axis_size("tp")
    n = nkv * ntp
    tokens, state, strength = args[0], args[16], args[10]
    rows, cols = tokens.shape
    seqs, heads, hd, _ = state.shape
    if cols % 128 or ntp < 2 or nkv < 2 or seqs * heads > hd or seqs % 8:
        return shards_plain(*args)
    args = [a.reshape(1, -1) if a.ndim == 1 else a for a in args]
    for at in (2, 3, 10, 11, 14, 19, 20):
        args[at] = args[at].T
    width = heads * hd
    buffers = [pltpu.VMEM(a.shape, a.dtype) for a in args[1:]]
    buffers += [pltpu.VMEM((n, rows, cols), BF16)] * 3
    buffers += [pltpu.VMEM((n - 1, rows, cols), BF16)] * 4
    buffers += [
        pltpu.VMEM((nkv, seqs, 4 * width), BF16),
        pltpu.VMEM((nkv - 1, seqs, 4 * width), BF16),
        pltpu.VMEM((nkv, seqs, width), BF16),
        pltpu.VMEM((ntp - 1, rows, cols), BF16),
        pltpu.VMEM((ntp - 1, rows, cols), BF16),
        pltpu.VMEM((nkv, seqs, 128), F32),
        pltpu.VMEM((n - 1, seqs, 128), F32),
        pltpu.VMEM((heads, seqs // 2, 2 * hd, 2 * hd), BF16),
        pltpu.VMEM((heads, seqs, hd), F32),
        pltpu.VMEM((heads, seqs, hd), F32),
        pltpu.VMEM(state.shape, F32),
        pltpu.VMEM((rows, cols), BF16),
        pltpu.SemaphoreType.DMA((len(args),)),
        pltpu.SemaphoreType.DMA((2,)),
        pltpu.SemaphoreType.DMA((9, n)),
        pltpu.SemaphoreType.DMA((9, n)),
    ]
    results = pl.pallas_call(
        functools.partial(layer_kernel, nkv, ntp),
        out_shape=(
            jax.ShapeDtypeStruct(tokens.shape, tokens.dtype),
            jax.ShapeDtypeStruct(state.shape, state.dtype),
        ),
        in_specs=[pl.BlockSpec(memory_space=pl.ANY)] * len(args),
        out_specs=[pl.BlockSpec(memory_space=pl.ANY)] * 2,
        scratch_shapes=buffers,
        compiler_params=pltpu.CompilerParams(
            collective_id=0, has_side_effects=True, vmem_limit_bytes=60 * 1024 * 1024
        ),
    )(*args)
    pieces = 8 if seqs % 8 == 0 else 1
    return pl.pallas_call(
        hand_over,
        out_shape=(
            jax.ShapeDtypeStruct(tokens.shape, tokens.dtype),
            jax.ShapeDtypeStruct(state.shape, state.dtype),
        ),
        in_specs=[pl.BlockSpec(memory_space=pl.ANY)] * 2,
        out_specs=[pl.BlockSpec(memory_space=pl.ANY)] * 2,
        scratch_shapes=[
            pltpu.VMEM(tokens.shape, tokens.dtype),
            pltpu.VMEM(state.shape, state.dtype),
            pltpu.SemaphoreType.DMA((pieces + 1,)),
            pltpu.SemaphoreType.DMA((pieces + 1,)),
        ],
        compiler_params=pltpu.CompilerParams(vmem_limit_bytes=60 * 1024 * 1024),
    )(*results)


def solution(mesh):
    placed = (
        P("dp", ("kv", "tp")),
        P(),
        P(None, ("kv", "tp")),
        P(None, ("kv", "tp")),
        P(("kv", "tp"), None),
        P(),
        P("kv", "tp"),
        P("kv", "tp"),
        P("kv", "tp"),
        P("kv", "tp"),
        P(),
        P(),
        P(),
        P(),
        P(("dp", "kv"), "tp"),
        P(),
        P(("dp", "kv"), "tp", None, None),
        P("tp", "kv"),
        P(),
        P(None, ("kv", "tp")),
        P(None, ("kv", "tp")),
        P(("kv", "tp"), None),
    )
    return jax.shard_map(
        shards,
        mesh=mesh,
        in_specs=placed,
        out_specs=(P("dp", ("kv", "tp")), P(("dp", "kv"), "tp", None, None)),
        check_vma=False,
    )
```
